32 devices in a mesh: grp: 2 (over y), kv: 4 (over z), tp: 4 (over x, core).
Axes of the slice: x: 2, y: 2, z: 4, core: 2. Of those that a mesh axis runs over, the one named last changes fastest.
Arguments:
- stream: bfloat16 [16, 4096], P('grp', 'kv'), parts along dimension 0, may hold values from -6 to 6
- attn_gain: bfloat16 [4096], P('kv'), may hold values from 0.099609375 to 1.8984375
- query_weight: bfloat16 [4096, 4096], P('kv', 'tp'), may hold values from -0.09375 to 0.09375
- query_gain: float32 [64], replicated, may hold values from 0.1 to 1.9
- key_cache: bfloat16 [16, 2048, 1024], P('grp', 'kv', 'tp'), parts along dimension 0, may hold values from -200 to 200
- value_cache: bfloat16 [16, 2048, 1024], P('grp', 'kv', 'tp'), parts along dimension 0, may hold values from -6 to 6
- gate_cache: float32 [16, 16, 2048], P('grp', 'tp', 'kv'), parts along dimension 0, may hold values from -2048 to 0, as said below
- output_weight: bfloat16 [4096, 4096], P('tp', 'kv'), may hold values from -0.75 to 0.75
- mixer_gain: bfloat16 [4096], replicated, may hold values from 0.099609375 to 1.8984375
- up_weight: bfloat16 [16384, 4096], P(('kv', 'tp')), may hold values from -0.09375 to 0.09375
- down_weight: bfloat16 [16384, 4096], P(('kv', 'tp')), may hold values from -0.0625 to 0.0625
Outputs:
- result: bfloat16 [16, 4096], P('grp', ('kv', 'tp')), parts along dimension 0
The draws below stay inside these ranges and needn't reach their ends.
There are 2 independent parts, one for each index of `grp`. The reference program is written for one: setup_inputs(seed, part) draws one part's arguments, and reference() takes and returns one part's arrays. A program takes and returns all parts, laid end to end along the dimension named above; an argument that names none is the same for every part. Nothing has to cross between parts.
Inputs may be any that keep to these rules, and one draw needn't show every extreme that they name: `gate_cache`: cumulative log forget gates: along positions each row never rises.
All inputs are finite; a program needn't handle non-finite values.
Results may differ from the reference program's by a relative error of at most 0.007.
The reference program's roundings to bfloat16 on the way (of `scaled`, `queries`, `attended`, `residual`, `normed` and `squared`) count: a program that leaves them out, or rounds other values in their place, can miss the bound.
Values may be sent and summed in bfloat16 or wider, within the bound.
No kernel may reach another device: no remote copies, remote signals or barrier semaphores. Data moves between devices by JAX's collectives and lax.ppermute only.
A program may use at most 64 MiB of HBM per device.

```python
import jax
import jax.numpy as jnp
from jax import lax

D = 4096
HEAD_DIM = 64
HEADS = 64
KEY_VALUE_HEADS = 16
FF = 16384
POS_DEV = 512
SEQUENCE_COUNT = 8
CACHED_POSITIONS = 2048
N_KV = 4


def draw_key_cache(key, part):
    width = KEY_VALUE_HEADS * HEAD_DIM
    key_rows = jax.random.split(key, 1)
    base = 2.0 * jax.random.normal(key_rows[0], (SEQUENCE_COUNT, CACHED_POSITIONS, width), jnp.float32)
    return jnp.clip(base, -200.0, 200.0).astype(jnp.bfloat16)


def draw_gate_cache(key, part):
    key_rows = jax.random.split(key, 5)
    fast_flag = jax.random.randint(key_rows[0], (1, KEY_VALUE_HEADS, 1), 0, 2) == 1
    blocks = CACHED_POSITIONS // POS_DEV
    block_rate = jnp.exp(jax.random.uniform(key_rows[1], (SEQUENCE_COUNT, KEY_VALUE_HEADS, blocks, 1), jnp.float32, -0.7, 0.7))
    block_rate = jnp.broadcast_to(block_rate, (SEQUENCE_COUNT, KEY_VALUE_HEADS, blocks, POS_DEV)).reshape(SEQUENCE_COUNT, KEY_VALUE_HEADS, CACHED_POSITIONS)
    jitter = jax.random.uniform(key_rows[2], (SEQUENCE_COUNT, KEY_VALUE_HEADS, CACHED_POSITIONS), jnp.float32, 0.3, 1.7)
    rate = jnp.where(fast_flag, 1.0 / 40.0, 1.0 / CACHED_POSITIONS)
    step_history = -rate * block_rate * jitter
    group_sites = jax.random.randint(key_rows[3], (SEQUENCE_COUNT, KEY_VALUE_HEADS, 3, 1), 0, CACHED_POSITIONS)
    group_length = jnp.log(jax.random.uniform(key_rows[4], (SEQUENCE_COUNT, KEY_VALUE_HEADS, 3, 1), jnp.float32, 0.5, 0.8))
    position_index = jnp.arange(CACHED_POSITIONS, dtype=jnp.int32)[None, None, None, :]
    position_groups = jnp.sum(jnp.where(position_index == group_sites, group_length, 0.0), axis=2)
    return jnp.cumsum(step_history + position_groups, axis=-1).astype(jnp.float32)


def strengthened(drawn, rng, source, target, blocks, factor):
    owner, partner = [(jnp.arange(drawn.shape[dim]) // (drawn.shape[dim] // blocks)).reshape([-1 if axis == dim else 1 for axis in range(drawn.ndim)]) for dim in (source, target)]
    chosen = jax.random.permutation(rng, blocks)[partner]
    strong = (owner == chosen) | (owner == (partner + blocks // 2) % blocks)
    return jnp.where(strong, factor * drawn, drawn)


def block_levels(stream_key, dims, cuts, least, largest):
    loudness = 1.0
    for position, parts in cuts:
        draws = jax.random.uniform(jax.random.fold_in(jax.random.fold_in(stream_key, 6), position), (parts,), jnp.float32, least / len(cuts), largest / len(cuts))
        loudness = loudness * jnp.repeat(jnp.exp(draws), dims[position] // parts).reshape((-1,) + (1,) * (len(dims) - 1 - position))
    return loudness


def scatter_about(rng, extent, deviation, most, cuts=(), kind=jnp.bfloat16):
    values = jax.random.normal(rng, extent, jnp.float32) * deviation
    if len(cuts) > 0:
        values = block_levels(rng, extent, cuts, -0.22, 0.18) * values
    return jnp.clip(values, min=-most, max=most).astype(kind)


def gaussian_with(own_key, dims, scale, limit, cuts, heavy, held_as=jnp.bfloat16):
    values = scale * jax.random.normal(own_key, dims, jnp.float32)
    if cuts:
        values = values * block_levels(own_key, dims, cuts, -0.22, 0.18)
    return jnp.clip(strengthened(values, jax.random.fold_in(own_key, 3), *heavy), -limit, limit).astype(held_as)


def setup_inputs(seed: int = 0, part: int = 0) -> dict:
    key_list = jax.random.split(jax.random.key(seed), 12)
    own_keys = jax.random.split(jax.random.fold_in(key_list[11], part), 12)
    return {
        "stream": scatter_about(own_keys[0], (SEQUENCE_COUNT, D), 1.0, 6.0, ((1, 4),)),
        "attn_gain": jnp.clip(1.0 + 0.18 * jax.random.normal(key_list[1], (D,), jnp.float32), 0.099609375, 1.8984375).astype(jnp.bfloat16),
        "query_weight": scatter_about(key_list[2], (D, HEADS * HEAD_DIM), D ** -0.5, 0.09375, ((0, 4), (1, 4))),
        "query_gain": jnp.clip(1.0 + 0.18 * jax.random.normal(key_list[3], (HEAD_DIM,), jnp.float32), 0.1, 1.9),
        "key_cache": draw_key_cache(jax.random.fold_in(jax.random.fold_in(key_list[11], part), 71), part),
        "value_cache": scatter_about(own_keys[5], (SEQUENCE_COUNT, CACHED_POSITIONS, KEY_VALUE_HEADS * HEAD_DIM), 1.0, 6.0, ((1, 4), (2, 4))),
        "gate_cache": draw_gate_cache(jax.random.fold_in(jax.random.fold_in(key_list[11], part), 71), part),
        "output_weight": scatter_about(key_list[7], (HEADS * HEAD_DIM, D), 0.125, 0.75, ((0, 4), (1, 4))),
        "mixer_gain": jnp.clip(1.0 + 0.18 * jax.random.normal(key_list[8], (D,), jnp.float32), 0.099609375, 1.8984375).astype(jnp.bfloat16),
        "up_weight": scatter_about(key_list[9], (FF, D), D ** -0.5, 0.09375, ((0, 16),)),
        "down_weight": gaussian_with(key_list[10], (FF, D), FF ** -0.5, 0.0625, ((0, 16),), (0, 1, 16, 2.0)),
    }


EPS = 1e-06

def rms_scale(values):
    return lax.rsqrt(lax.optimization_barrier(jnp.mean(values * values, axis=-1, keepdims=True)) + EPS)

def block_attention(queries, key_block, value_block, gate_block):
    batch_rows, position_index = (key_block.shape[0], key_block.shape[1])
    kv_local = queries.shape[1]
    key_heads = key_block.reshape(batch_rows, position_index, kv_local, HEAD_DIM).astype(jnp.float32)
    value_heads = value_block.reshape(batch_rows, position_index, kv_local, HEAD_DIM).astype(jnp.float32)
    scores = jnp.einsum('skgd,spkd->skgp', queries.astype(jnp.float32), key_heads) * HEAD_DIM ** (-0.5)
    scores = scores - gate_block[:, :, None, :]
    score_top = lax.optimization_barrier(jnp.max(scores, axis=-1))
    weights_exp = jnp.exp(scores - score_top[..., None])
    totals = lax.optimization_barrier(jnp.sum(weights_exp, axis=-1))
    rounded = weights_exp.astype(jnp.bfloat16).astype(jnp.float32)
    weighted = jnp.einsum('skgp,spkd->skgd', rounded, value_heads)
    return (score_top, totals, weighted)

def reference(stream, attn_gain, query_weight, query_gain, key_cache, value_cache, gate_cache, output_weight, mixer_gain, up_weight, down_weight):
    scaled = (stream.astype(jnp.float32) * attn_gain.astype(jnp.float32)).astype(jnp.bfloat16)
    query_raw = jnp.dot(scaled, query_weight, preferred_element_type=jnp.float32)
    query_heads = query_raw.reshape(SEQUENCE_COUNT, HEADS, HEAD_DIM)
    queries = (query_heads * rms_scale(query_heads) * query_gain).astype(jnp.bfloat16)
    queries = queries.reshape(SEQUENCE_COUNT, KEY_VALUE_HEADS, HEADS // KEY_VALUE_HEADS, HEAD_DIM)
    key_blocks = key_cache.reshape(SEQUENCE_COUNT, N_KV, POS_DEV, KEY_VALUE_HEADS * HEAD_DIM).swapaxes(0, 1)
    value_blocks = value_cache.reshape(SEQUENCE_COUNT, N_KV, POS_DEV, KEY_VALUE_HEADS * HEAD_DIM).swapaxes(0, 1)
    gate_blocks = gate_cache.reshape(SEQUENCE_COUNT, KEY_VALUE_HEADS, N_KV, POS_DEV).transpose(2, 0, 1, 3)

    def one_block(pieces):
        return block_attention(queries, pieces[0], pieces[1], pieces[2])
    score_top, totals, weighted = lax.map(one_block, (key_blocks, value_blocks, gate_blocks))
    best = lax.optimization_barrier(jnp.max(score_top, axis=0))
    factor = jnp.exp(score_top - best[None])
    totals = lax.optimization_barrier(jnp.sum(factor * totals, axis=0))
    weighted = lax.optimization_barrier(jnp.sum(factor[..., None] * weighted, axis=0))
    attended = (weighted / totals[..., None]).reshape(SEQUENCE_COUNT, HEADS * HEAD_DIM).astype(jnp.bfloat16)
    projected = jnp.dot(attended, output_weight, preferred_element_type=jnp.float32)
    residual = (stream.astype(jnp.float32) + projected).astype(jnp.bfloat16)
    residual_f = residual.astype(jnp.float32)
    normed = (residual_f * rms_scale(residual_f) * mixer_gain.astype(jnp.float32)).astype(jnp.bfloat16)
    up_proj = lax.dot_general(normed, up_weight, (((1,), (1,)), ((), ())), preferred_element_type=jnp.float32)
    squared = jnp.square(jax.nn.relu(up_proj)).astype(jnp.bfloat16)
    down_proj = jnp.dot(squared, down_weight, preferred_element_type=jnp.float32)
    return (residual_f + down_proj).astype(jnp.bfloat16)
```

```python
import functools

import jax
import jax.numpy as jnp
from jax import lax
from jax.experimental import pallas as pl
from jax.experimental.pallas import tpu as pltpu
from jax.sharding import PartitionSpec as P

HEAD_DIM = 64
EPS = 1e-06
LANES = 128
F32 = jnp.float32
BF16 = jnp.bfloat16
NT = (((1,), (1,)), ((), ()))
MIB = 1024 * 1024


def call(kernel, out_shape, args, scratch=(), limit=8):
    nbytes = sum(a.size * a.dtype.itemsize for a in args)
    return pl.pallas_call(
        kernel,
        out_shape=out_shape,
        in_specs=[pl.BlockSpec(memory_space=pltpu.VMEM)] * len(args),
        out_specs=pl.BlockSpec(memory_space=pltpu.VMEM),
        scratch_shapes=list(scratch),
        compiler_params=pltpu.CompilerParams(vmem_limit_bytes=limit * MIB),
        cost_estimate=pl.CostEstimate(flops=10**10, bytes_accessed=nbytes, transcendentals=0),
        name=kernel.__name__ if hasattr(kernel, "__name__") else kernel.func.__name__,
    )(*args)


def exchange(value, axis, size):
    return [
        lax.ppermute(value, axis, [(i, i ^ step) for i in range(size)])
        for step in range(1, size)
    ]


def tree_sum(terms):
    while len(terms) > 1:
        terms = [a + b for a, b in zip(terms[::2], terms[1::2])]
    return terms[0]


def query_kernel(stream_ref, gain_ref, weight_ref, out_ref):
    scaled = (stream_ref[...].astype(F32) * gain_ref[...].astype(F32)).astype(BF16)
    out_ref[...] = jnp.dot(scaled, weight_ref[...], preferred_element_type=F32)


def attention_kernel(count, kv_local, *refs):
    parts, (gain_ref, key_ref, value_ref, gate_ref, out_ref, wide_ref) = refs[:count], refs[count:]
    rows = out_ref.shape[0]
    width = kv_local * HEAD_DIM
    group = rows // key_ref.shape[0]
    heads = group * kv_local
    batch = key_ref.shape[0]
    raw = tree_sum([ref[...] for ref in parts])
    lane = lax.broadcasted_iota(jnp.int32, (batch, LANES), 1)
    low = lane < HEAD_DIM
    gain = jnp.concatenate([gain_ref[...]] * 2, axis=1)
    zero = jnp.zeros((batch, LANES), F32)
    for pair in range(heads // 2):
        vec = raw[:, pair * LANES : (pair + 1) * LANES]
        square = vec * vec
        sums = [
            jnp.sum(jnp.where(mask, square, 0.0), axis=1, keepdims=True)
            for mask in (low, jnp.logical_not(low))
        ]
        scales = [lax.rsqrt(s * (1.0 / HEAD_DIM) + EPS) for s in sums]
        query = (vec * jnp.where(low, scales[0], scales[1])) * gain
        swapped = pltpu.roll(query, HEAD_DIM, 1)
        for half in range(2):
            head = pair * 2 + half
            kv_head = head // group
            source = query if half == kv_head % 2 else swapped
            placed = jnp.where(low if kv_head % 2 == 0 else jnp.logical_not(low), source, 0.0)
            for column in range(width // LANES):
                block = placed if column == kv_head // 2 else zero
                wide_ref[column, head * batch : (head + 1) * batch, :] = block
    positions = key_ref.shape[1]
    head_row = lax.broadcasted_iota(jnp.int32, (heads, width), 0) // group
    own = head_row == lax.broadcasted_iota(jnp.int32, (heads, width), 1) // HEAD_DIM
    stat_row = lax.broadcasted_iota(jnp.int32, (heads, LANES), 0) // group
    stat_lane = lax.broadcasted_iota(jnp.int32, (heads, LANES), 1)
    for s in range(batch):
        query = jnp.concatenate(
            [
                wide_ref[column, pl.ds(s, heads, stride=batch), :]
                for column in range(width // LANES)
            ],
            axis=1,
        ).astype(BF16)
        scores = lax.dot_general(query, key_ref[s], NT, preferred_element_type=F32)
        gate = jnp.concatenate(
            [
                jnp.broadcast_to(gate_ref[s, k : k + 1, :], (group, positions))
                for k in range(kv_local)
            ],
            axis=0,
        )
        scores = scores * HEAD_DIM ** (-0.5) - gate
        top = jnp.max(scores, axis=1, keepdims=True)
        probs = jnp.exp(scores - top)
        total = jnp.sum(probs, axis=1, keepdims=True)
        weighted = jnp.dot(probs.astype(BF16), value_ref[s], preferred_element_type=F32)
        weighted = jnp.where(own, weighted, 0.0)
        stats = jnp.where(stat_lane == stat_row, top, 0.0)
        stats = stats + jnp.where(stat_lane == stat_row + kv_local, total, 0.0)
        row = jnp.concatenate([weighted, stats], axis=1)
        out_ref[s * group : (s + 1) * group, :] = tree_sum(
            [row[k * group : (k + 1) * group] for k in range(kv_local)]
        )


def project_kernel(count, kv_local, *refs):
    parts, (weight_ref, out_ref, attended_ref) = refs[:count], refs[count:]
    width = kv_local * HEAD_DIM
    rows = parts[0].shape[0]
    batch = out_ref.shape[0]
    group = rows // batch
    stats = [ref[:, width:] for ref in parts]
    best = functools.reduce(jnp.maximum, stats)
    factors = [jnp.exp(s - best) for s in stats]
    totals = sum(f * pltpu.roll(s, LANES - kv_local, 1) for f, s in zip(factors, stats))
    block = lax.broadcasted_iota(jnp.int32, (rows, width), 1) // HEAD_DIM

    def expand(narrow):
        wide = jnp.broadcast_to(narrow[:, 0:1], (rows, width))
        for k in range(1, kv_local):
            wide = jnp.where(block == k, narrow[:, k : k + 1], wide)
        return wide

    weighted = sum(expand(f) * ref[:, :width] for f, ref in zip(factors, parts))
    attended = weighted / expand(totals)
    for column in range(width // LANES):
        attended_ref[column] = attended[:, column * LANES : (column + 1) * LANES]
    acc = None
    for g in range(group):
        attended = jnp.concatenate(
            [
                attended_ref[column, pl.ds(g, batch, stride=group), :]
                for column in range(width // LANES)
            ],
            axis=1,
        ).astype(BF16)
        weight = jnp.concatenate(
            [
                weight_ref[(k * group + g) * HEAD_DIM : (k * group + g + 1) * HEAD_DIM, :]
                for k in range(kv_local)
            ],
            axis=0,
        )
        term = jnp.dot(attended, weight, preferred_element_type=F32)
        acc = term if acc is None else acc + term
    out_ref[...] = acc


def mixer_kernel(count, *refs):
    parts, (gain_ref, up_ref, down_ref, out_ref, rows_ref) = refs[:count], refs[count:]
    chunk = parts[0].shape[1]
    model = rows_ref.shape[1]
    index = lax.axis_index("kv") if count > 1 else 0
    for step, ref in enumerate(parts):
        start = pl.multiple_of(jnp.bitwise_xor(index, step) * chunk, LANES)
        rows_ref[:, pl.ds(start, chunk)] = ref[...].astype(F32)
    rows = rows_ref[...]
    scale = lax.rsqrt(jnp.mean(rows * rows, axis=1, keepdims=True) + EPS)
    normed = (rows * scale * gain_ref[...].astype(F32)).astype(BF16)
    hidden = up_ref.shape[0]
    tile = 256
    squared = []
    for start in range(0, hidden, tile):
        pre = lax.dot_general(
            up_ref[start : start + tile, :], normed, NT, preferred_element_type=F32
        )
        squared.append(jnp.square(jnp.maximum(pre, 0.0)).T.astype(BF16))
    squared = jnp.concatenate(squared, axis=1)
    blocks, _, width = out_ref.shape
    for b in range(blocks):
        out_ref[b] = jnp.dot(
            squared, down_ref[:, b * width : (b + 1) * width], preferred_element_type=F32
        ).astype(out_ref.dtype)


def per_device(
    kv_size,
    tp_size,
    stream,
    attn_gain,
    query_weight,
    query_gain,
    key_cache,
    value_cache,
    gate_cache,
    output_weight,
    mixer_gain,
    up_weight,
    down_weight,
):
    batch, chunk = stream.shape
    heads_width = query_weight.shape[1]
    kv_local = key_cache.shape[2] // HEAD_DIM
    heads_local = heads_width // HEAD_DIM
    group = heads_local // kv_local
    width = kv_local * HEAD_DIM

    def shape(dims, dtype):
        return jax.ShapeDtypeStruct(dims, dtype)

    partial = call(
        query_kernel,
        shape((batch, heads_width), F32),
        (stream, attn_gain[None], query_weight),
    )
    if kv_size <= 4:
        queries = [partial] + exchange(partial, "kv", kv_size)
    else:
        queries = [lax.psum(partial, "kv")]
    mine = call(
        functools.partial(attention_kernel, len(queries), kv_local),
        shape((batch * group, width + LANES), F32),
        (*queries, query_gain[None], key_cache, value_cache, gate_cache),
        scratch=[pltpu.VMEM((width // LANES, heads_local * batch, LANES), F32)],
    )
    if kv_size <= 4:
        blocks = [mine] + exchange(mine, "kv", kv_size)
    else:
        gathered = lax.all_gather(mine, "kv")
        blocks = [gathered[i] for i in range(kv_size)]
    projected = call(
        functools.partial(project_kernel, len(blocks), kv_local),
        shape((batch, output_weight.shape[1]), F32),
        (*blocks, output_weight),
        scratch=[pltpu.VMEM((width // LANES, batch * group, LANES), F32)],
    )
    if tp_size <= 4:
        projected = tree_sum([projected] + exchange(projected, "tp", tp_size))
    else:
        projected = lax.psum(projected, "tp")
    residual = (stream.astype(F32) + projected).astype(BF16)
    if kv_size <= 4:
        chunks = [residual] + exchange(residual, "kv", kv_size)
    else:
        chunks = [lax.all_gather(residual, "kv", axis=1, tiled=True)]
    devices = kv_size * tp_size
    model = down_weight.shape[1]
    own_width = model // devices
    partials = call(
        functools.partial(mixer_kernel, len(chunks)),
        shape((devices, batch, own_width), F32),
        (*chunks, mixer_gain[None], up_weight, down_weight),
        scratch=[pltpu.VMEM((batch, model), F32)],
        limit=20,
    )
    arrived = lax.all_to_all(partials, ("kv", "tp"), 0, 0)
    own = lax.dynamic_slice_in_dim(residual, lax.axis_index("tp") * own_width, own_width, 1)
    return (own.astype(F32) + jnp.sum(arrived, axis=0)).astype(BF16)


def solution(mesh):
    in_specs = (
        P("grp", "kv"),
        P("kv"),
        P("kv", "tp"),
        P(),
        P("grp", "kv", "tp"),
        P("grp", "kv", "tp"),
        P("grp", "tp", "kv"),
        P("tp", "kv"),
        P(),
        P(("kv", "tp"), None),
        P(("kv", "tp"), None),
    )
    out_specs = P("grp", ("kv", "tp"))
    return jax.shard_map(
        functools.partial(per_device, mesh.shape["kv"], mesh.shape["tp"]),
        mesh=mesh,
        in_specs=in_specs,
        out_specs=out_specs,
        check_vma=False,
    )
```
